256 devices in a mesh: grp: 2 (over y), ep: 32 (over z, core), tp: 4 (over x).
Axes of the slice: x: 4, y: 2, z: 16, core: 2. Of those that a mesh axis runs over, the one named last changes fastest.
The devices are a block of a 4x16x16 slice.
Arguments:
- mixer_tokens: bfloat16 [32768, 2048], P(('grp', 'ep', 'tp')), parts along dimension 0, may hold values from -6 to 6
- mixer_gain: float32 [2048], replicated, may hold values from 0.1 to 1.9
- proj_in: bfloat16 [2048, 1024], P(None, 'tp'), may hold values from -0.125 to 0.125
- pool_weight: bfloat16 [4, 256, 256], P('tp'), may hold values from -0.375 to 0.375
- pool_scale: float32 [1024], P('tp'), may hold values from 0.1 to 1.9
- proj_out: bfloat16 [1024, 2048], P('tp'), may hold values from -0.1875 to 0.1875
- expert_tokens: bfloat16 [32768, 2048], P(('grp', 'ep', 'tp')), parts along dimension 0, may hold values from -6 to 6
- expert_gain: float32 [2048], replicated, may hold values from 0.1 to 1.9
- expert_route: int32 [32768, 2], P(('grp', 'ep')), parts along dimension 0, may hold values from 0 to 63, as said below
- route_gate: float32 [32768, 2], P(('grp', 'ep')), parts along dimension 0, may hold values from 0.1 to 1
- expert_gate: bfloat16 [64, 2048, 1024], P('ep', None, 'tp'), may hold values from -0.125 to 0.125
- expert_up: bfloat16 [64, 2048, 1024], P('ep', None, 'tp'), may hold values from -0.125 to 0.125
- expert_down: bfloat16 [64, 1024, 2048], P('ep', 'tp'), may hold values from -0.1875 to 0.1875
Outputs:
- mixed_rows: bfloat16 [32768, 2048], P(('grp', 'ep', 'tp')), parts along dimension 0
- moe_rows: bfloat16 [32768, 2048], P(('grp', 'ep', 'tp')), parts along dimension 0
The draws below stay inside these ranges and needn't reach their ends.
There are 2 independent parts, one for each index of `grp`. The reference program is written for one: setup_inputs(seed, part) draws one part's arguments, and reference() takes and returns one part's arrays. A program takes and returns all parts, laid end to end along the dimension named above; an argument that names none is the same for every part. Nothing has to cross between parts.
Inputs may be any that keep to these rules, and one draw needn't show every extreme that they name: `expert_route`: each row names two different experts of one group of 4 consecutive experts. In each aligned block of 128 rows (the routes of the tokens that lie on one device) no expert is named by more than 8 rows, and every expert of a group that the block names at all is named by exactly 8 of its rows; one group, the same in every block, is named in every block, and which other groups a block names varies from block to block.
All inputs are finite; a program needn't handle non-finite values.
Results may differ from the reference program's by a relative error of at most 0.011.
Values may be sent and summed in bfloat16 or wider, within the bound.
No kernel may reach another device: no remote copies, remote signals or barrier semaphores. Data moves between devices by JAX's collectives and lax.ppermute only.
A program may use at most 128 MiB of HBM per device.

```python
import jax
import jax.numpy as jnp
from jax import lax

D = 2048
POOL_WIDTH = 1024
POOL_GROUPS = 4
HIDDEN_SIZE = 1024
GROUP_SIZE = 4
TOK_DEV = 128
EXPERTS = 64
GROUPS = 16
CAP = 8
TOKENS = 16384
N_EP = 32
N_TP = 4


def draw_expert_route(key, part):
    blocks = TOKENS // TOK_DEV
    unit = TOK_DEV // GROUPS
    hot_key, cold_key, label_key, order_key = jax.random.split(jax.random.fold_in(key, 17), 4)
    hot_group = jax.random.randint(hot_key, (), 0, GROUPS)
    cold_keys = jax.random.split(cold_key, blocks)
    cold_order = jax.vmap(lambda single: jax.random.permutation(single, GROUPS - 1))(cold_keys).astype(jnp.int32)
    position = jnp.arange(TOK_DEV, dtype=jnp.int32)
    unit_index = position // unit
    within = position % unit
    pair_index = jnp.maximum((unit_index - 2) // 2, 0)
    cold_pick = jnp.take_along_axis(cold_order, jnp.broadcast_to(pair_index[None, :], (blocks, TOK_DEV)), axis=1)
    group_id = jnp.where(unit_index[None, :] < 2, hot_group, (hot_group + 1 + cold_pick) % GROUPS)
    member = unit_index % 2 * unit + within
    first_pick = member % GROUP_SIZE
    second_pick = (member + 1) % GROUP_SIZE
    label_keys = jax.random.split(label_key, blocks * GROUPS)
    labels = jax.vmap(lambda single: jax.random.permutation(single, GROUP_SIZE))(label_keys).reshape(blocks, GROUPS, GROUP_SIZE).astype(jnp.int32)
    group_labels = jnp.take_along_axis(labels, group_id[:, :, None], axis=1)
    first_label = jnp.take_along_axis(group_labels, jnp.broadcast_to(first_pick[None, :, None], (blocks, TOK_DEV, 1)), axis=2)[:, :, 0]
    second_label = jnp.take_along_axis(group_labels, jnp.broadcast_to(second_pick[None, :, None], (blocks, TOK_DEV, 1)), axis=2)[:, :, 0]
    routes = jnp.stack([group_id * GROUP_SIZE + first_label, group_id * GROUP_SIZE + second_label], axis=-1)
    order_keys = jax.random.split(order_key, blocks)
    orders = jax.vmap(lambda single: jax.random.permutation(single, TOK_DEV))(order_keys).astype(jnp.int32)
    shuffled = jnp.take_along_axis(routes, jnp.broadcast_to(orders[:, :, None], (blocks, TOK_DEV, 2)), axis=1)
    return shuffled.reshape(TOKENS, 2).astype(jnp.int32)


def steps_of(rng, extent, shards, low, top_value):
    gain = 1.0
    for dim, blocks in shards:
        steps = jax.random.uniform(jax.random.fold_in(jax.random.fold_in(rng, 6), dim), (blocks,), jnp.float32, low / len(shards), top_value / len(shards))
        gain = gain * jnp.repeat(jnp.exp(steps), extent[dim] // blocks).reshape((-1,) + (1,) * (len(extent) - 1 - dim))
    return gain


def scatter_about(key, dims, width, most, cuts=(), kind=jnp.bfloat16):
    drawn = jax.random.normal(key, dims, jnp.float32) * width
    if len(cuts) > 0:
        drawn = steps_of(key, dims, cuts, -0.22, 0.18) * drawn
    return jnp.clip(drawn, min=-most, max=most).astype(kind)


def setup_inputs(seed: int = 0, part: int = 0) -> dict:
    streams_of = jax.random.split(jax.random.key(seed), 14)
    own_keys = jax.random.split(jax.random.fold_in(streams_of[13], part), 14)
    mixer_tokens = scatter_about(own_keys[0], (TOKENS, D), 1.0, 6.0, ((0, 128),))
    mixer_gain = jnp.clip(1.0 + 0.18 * jax.random.normal(streams_of[1], (D,), jnp.float32), 0.1, 1.9)
    proj_in = scatter_about(streams_of[2], (D, POOL_WIDTH), D ** -0.5, 0.125, ((1, 4),))
    pool_weight = scatter_about(streams_of[3], (POOL_GROUPS, POOL_WIDTH // POOL_GROUPS, POOL_WIDTH // POOL_GROUPS), (POOL_WIDTH // POOL_GROUPS) ** -0.5, 0.375, ((0, 4),))
    pool_scale = jnp.clip(1.0 + 0.18 * jax.random.normal(streams_of[4], (POOL_WIDTH,), jnp.float32), 0.1, 1.9)
    proj_out = scatter_about(streams_of[5], (POOL_WIDTH, D), POOL_WIDTH ** -0.5, 0.1875, ((0, 4),))
    expert_tokens = scatter_about(own_keys[6], (TOKENS, D), 1.0, 6.0, ((0, 128),))
    expert_gain = jnp.clip(1.0 + 0.18 * jax.random.normal(streams_of[7], (D,), jnp.float32), 0.1, 1.9)
    expert_route = draw_expert_route(jax.random.fold_in(jax.random.fold_in(streams_of[13], part), 71), part)
    route_gate = jnp.clip(0.1 + 0.9 * jax.random.uniform(own_keys[9], (TOKENS, 2), jnp.float32) ** steps_of(own_keys[9], (TOKENS, 2), ((0, 32),), -0.2, 0.2), 0.1, 1.0)
    expert_gate = scatter_about(streams_of[10], (EXPERTS, D, HIDDEN_SIZE), D ** -0.5, 0.125, ((0, 32), (2, 4)))
    expert_up = scatter_about(streams_of[11], (EXPERTS, D, HIDDEN_SIZE), D ** -0.5, 0.125, ((0, 32), (2, 4)))
    expert_down = scatter_about(streams_of[12], (EXPERTS, HIDDEN_SIZE, D), HIDDEN_SIZE ** -0.5, 0.1875, ((0, 32), (1, 4)))
    return dict(mixer_tokens=mixer_tokens, mixer_gain=mixer_gain, proj_in=proj_in, pool_weight=pool_weight, pool_scale=pool_scale, proj_out=proj_out, expert_tokens=expert_tokens, expert_gain=expert_gain, expert_route=expert_route, route_gate=route_gate, expert_gate=expert_gate, expert_up=expert_up, expert_down=expert_down)


norm_eps = 1e-05
rim_rows = 15

def layer_norm(values, norm_gain):
    widened = values.astype(jnp.float32)
    center = lax.optimization_barrier(jnp.mean(widened, axis=-1, keepdims=True))
    spread = lax.optimization_barrier(jnp.mean(jnp.square(widened - center), axis=-1, keepdims=True))
    return ((widened - center) * lax.rsqrt(spread + norm_eps) * norm_gain).astype(jnp.bfloat16)

def pooled_diff(extended, windows, first_row):
    widened = extended.astype(jnp.float32)
    row_total = widened.shape[0] - rim_rows
    own_rows = widened[rim_rows:]
    window_sum = own_rows
    for offset in range(1, rim_rows + 1):
        lagged = widened[rim_rows - offset:rim_rows - offset + row_total]
        window_sum = window_sum + jnp.where(offset < windows[None, :], lagged, 0.0)
    position = first_row + jnp.arange(row_total, dtype=jnp.int32)
    covered = jnp.minimum(position[:, None] + 1, windows[None, :]).astype(jnp.float32)
    return (window_sum / covered - own_rows).astype(jnp.bfloat16)

def reference(mixer_tokens, mixer_gain, proj_in, pool_weight, pool_scale, proj_out, expert_tokens, expert_gain, expert_route, route_gate, expert_gate, expert_up, expert_down):
    mixer_norm = layer_norm(mixer_tokens, mixer_gain)
    projected = jnp.dot(mixer_norm, proj_in, preferred_element_type=jnp.float32).astype(jnp.bfloat16)
    group_width = POOL_WIDTH // POOL_GROUPS
    channel = jnp.arange(POOL_WIDTH, dtype=jnp.int32)
    windows = jnp.left_shift(jnp.full_like(channel, 2), channel // group_width)
    extended = jnp.concatenate([jnp.zeros((rim_rows, POOL_WIDTH), jnp.bfloat16), projected], axis=0)
    differences = pooled_diff(extended, windows, 0)
    grouped = differences.astype(jnp.float32).reshape(TOKENS, POOL_GROUPS, group_width)
    pool_mixed = jnp.einsum('tgc,gcd->tgd', grouped, pool_weight.astype(jnp.float32))
    pooled = (pool_mixed.reshape(TOKENS, POOL_WIDTH) * pool_scale).astype(jnp.bfloat16)
    block_width = POOL_WIDTH // N_TP
    out_total = jnp.zeros((TOKENS, D), jnp.float32)
    for block in range(N_TP):
        out_part = jnp.dot(pooled[:, block * block_width:(block + 1) * block_width], proj_out[block * block_width:(block + 1) * block_width], preferred_element_type=jnp.float32)
        out_total = out_total + lax.optimization_barrier(out_part.astype(jnp.bfloat16)).astype(jnp.float32)
    mixed_rows = out_total.astype(jnp.bfloat16)
    expert_norm = layer_norm(expert_tokens, expert_gain)
    flat_route = expert_route.reshape(-1).astype(jnp.int32)
    flat_gate = route_gate.reshape(-1)
    limit = N_EP * N_TP * CAP
    quarter = HIDDEN_SIZE // N_TP

    def expert_pass(carry, expert):
        chosen = flat_route == expert
        found = jnp.nonzero(chosen, size=limit, fill_value=0)[0].astype(jnp.int32)
        valid = jnp.arange(limit, dtype=jnp.int32) < jnp.sum(chosen.astype(jnp.int32))
        token_index = found // 2
        picked = expert_norm[token_index]
        gate_matrix = lax.dynamic_index_in_dim(expert_gate, expert, 0, keepdims=False)
        up_matrix = lax.dynamic_index_in_dim(expert_up, expert, 0, keepdims=False)
        down_matrix = lax.dynamic_index_in_dim(expert_down, expert, 0, keepdims=False)
        gate_part = jnp.dot(picked, gate_matrix, preferred_element_type=jnp.float32)
        up_part = jnp.dot(picked, up_matrix, preferred_element_type=jnp.float32)
        hidden = (jax.nn.silu(gate_part) * up_part).astype(jnp.bfloat16)
        summed = jnp.zeros((limit, D), jnp.float32)
        for block in range(N_TP):
            down_part = jnp.dot(hidden[:, block * quarter:(block + 1) * quarter], down_matrix[block * quarter:(block + 1) * quarter], preferred_element_type=jnp.float32)
            summed = summed + lax.optimization_barrier(down_part.astype(jnp.bfloat16)).astype(jnp.float32)
        expert_out = lax.optimization_barrier(summed.astype(jnp.bfloat16)).astype(jnp.float32)
        weight = jnp.where(valid, flat_gate[found], 0.0)
        carry = carry.at[token_index].add(weight[:, None] * expert_out)
        return (carry, None)
    moe_total, unused = lax.scan(expert_pass, jnp.zeros((TOKENS, D), jnp.float32), jnp.arange(EXPERTS, dtype=jnp.int32))
    moe_rows = moe_total.astype(jnp.bfloat16)
    return (mixed_rows, moe_rows)
```

```python
import jax
import jax.numpy as jnp
from jax import lax
from jax.sharding import PartitionSpec as P

GROUP_SIZE = 4


norm_eps = 1e-05
rim_rows = 15
chunks = 2


def shifted(value, axis, by):
    peers = lax.axis_size(axis)
    pairs = [(i, i + by) for i in range(peers) if 0 <= i + by < peers]
    return lax.ppermute(value, axis, pairs)


def copy_for_each(value, axis):
    peers = lax.axis_size(axis)
    return lax.all_to_all(
        jnp.broadcast_to(value[None], (peers, *value.shape)), axis, 0, 0, tiled=True
    )


def sum_at_owner(value, axis):
    peers = lax.axis_size(axis)
    blocks = value.reshape(peers, -1, value.shape[1])
    arrived = lax.all_to_all(blocks, axis, split_axis=0, concat_axis=0, tiled=True)
    return arrived.astype(jnp.float32).sum(axis=0)


def layer_norm(values, norm_gain):
    widened = values.astype(jnp.float32)
    center = jnp.mean(widened, axis=-1, keepdims=True)
    spread = jnp.mean(jnp.square(widened - center), axis=-1, keepdims=True)
    return ((widened - center) * lax.rsqrt(spread + norm_eps) * norm_gain).astype(jnp.bfloat16)


def pooled_diff(extended, windows, first_row):
    widened = extended.astype(jnp.float32)
    row_total = widened.shape[0] - rim_rows
    own_rows = widened[rim_rows:]
    window_sum = own_rows
    for offset in range(1, rim_rows + 1):
        lagged = widened[rim_rows - offset : rim_rows - offset + row_total]
        window_sum = window_sum + jnp.where(offset < windows[None, :], lagged, 0.0)
    position = first_row + jnp.arange(row_total, dtype=jnp.int32)
    covered = jnp.minimum(position[:, None] + 1, windows[None, :]).astype(jnp.float32)
    return (window_sum / covered - own_rows).astype(jnp.bfloat16)


def pool_mix(projected, pool_weight, pool_scale, windows, first_row):
    prior = shifted(projected[-rim_rows:], "ep", 1)
    differences = pooled_diff(jnp.concatenate([prior, projected], axis=0), windows, first_row)
    row_total, local_width = differences.shape
    grouped = differences.reshape(row_total, pool_weight.shape[0], pool_weight.shape[1])
    mixed_groups = jnp.einsum(
        "tgc,gcd->tgd", grouped, pool_weight, preferred_element_type=jnp.float32
    )
    return (mixed_groups.reshape(row_total, local_width) * pool_scale).astype(jnp.bfloat16)


def route_slots(routes, groups, packet):
    rows = routes.shape[1]
    group = routes[:, :, 0] // GROUP_SIZE
    named = group[:, :, None] == jnp.arange(groups, dtype=jnp.int32)
    order = jnp.arange(rows, dtype=jnp.int32)
    before = (order[:, None] > order[None, :]).astype(jnp.bfloat16)
    earlier = jnp.einsum(
        "tu,bug->btg", before, named.astype(jnp.bfloat16), preferred_element_type=jnp.float32
    )
    rank = jnp.sum(jnp.where(named, earlier, 0.0), axis=2).astype(jnp.int32)
    return group * packet + rank


def same_core(value, peers_per_group):
    peers = lax.axis_size("ep")
    rings = [list(range(c, peers, peers_per_group)) for c in range(peers_per_group)]
    return lax.all_to_all(value, "ep", 0, 0, axis_index_groups=rings, tiled=True)


def expert_rows(rows, weights, sets):
    total = None
    for (gate, up, down), weight in zip(sets, weights):
        parts = []
        for e in range(gate.shape[0]):
            gate_part = jnp.dot(rows, gate[e], preferred_element_type=jnp.float32)
            up_part = jnp.dot(rows, up[e], preferred_element_type=jnp.float32)
            parts.append(
                (jax.nn.silu(gate_part) * up_part * weight[:, e : e + 1]).astype(jnp.bfloat16)
            )
        hidden = jnp.concatenate(parts, axis=1)
        part = jnp.dot(
            hidden, down.reshape(-1, down.shape[2]), preferred_element_type=jnp.float32
        )
        total = part if total is None else total + part
    return total.astype(jnp.bfloat16)


def shards(
    mixer_tokens,
    mixer_gain,
    proj_in,
    pool_weight,
    pool_scale,
    proj_out,
    expert_tokens,
    expert_gain,
    expert_route,
    route_gate,
    expert_gate,
    expert_up,
    expert_down,
):
    ep_count = lax.axis_size("ep")
    tp_count = lax.axis_size("tp")
    tp_index = lax.axis_index("tp")
    ep_index = lax.axis_index("ep")
    own_count, model_width = mixer_tokens.shape
    local_width = proj_in.shape[1]
    group_width = pool_weight.shape[1]
    local_experts = expert_gate.shape[0]
    experts = local_experts * ep_count
    capacity = own_count * GROUP_SIZE // experts
    packet = capacity * GROUP_SIZE // 2
    groups = experts // GROUP_SIZE
    holders = GROUP_SIZE // local_experts
    place = ep_index % holders

    blocks = expert_route.reshape(tp_count, own_count, 2)
    slots = route_slots(blocks, groups, packet)
    member = blocks % GROUP_SIZE
    local = jnp.arange(GROUP_SIZE, dtype=jnp.int32)
    gates = route_gate.reshape(tp_count, own_count, 2)
    by_member = jnp.sum(
        jnp.where(member[:, :, :, None] == local, gates[:, :, :, None], 0.0), axis=2
    )
    slot_range = jnp.arange(groups * packet, dtype=jnp.int32)
    placed = slots[:, :, None] == slot_range
    slot_weight = jnp.einsum(
        "btj,bts->bjs",
        by_member,
        placed.astype(jnp.float32),
        precision=lax.Precision.HIGHEST,
        preferred_element_type=jnp.float32,
    )
    slot_weight = slot_weight.reshape(tp_count, GROUP_SIZE, groups, packet)
    slot_weight = slot_weight.transpose(2, 0, 1, 3).reshape(groups, -1)
    weights = same_core(slot_weight, holders).reshape(groups, tp_count, GROUP_SIZE, packet)
    weights = weights.transpose(1, 0, 3, 2)

    own_slots = lax.dynamic_index_in_dim(slots, tp_index, 0, keepdims=False)
    pick = (own_slots[:, None] == slot_range).astype(jnp.bfloat16)
    normed_expert = layer_norm(expert_tokens, expert_gain)
    outgoing = jnp.einsum(
        "ts,td->sd", pick, normed_expert, preferred_element_type=jnp.float32
    ).astype(jnp.bfloat16)
    outgoing = outgoing.reshape(groups, packet, model_width)

    own_set = (expert_gate, expert_up, expert_down)
    sets = [own_set]
    for s in range(1, holders):
        pairs = [(i, i - i % holders + (i + s) % holders) for i in range(ep_count)]
        sets.append(tuple(lax.ppermute(w, "ep", pairs) for w in own_set))

    normed_mixer = layer_norm(mixer_tokens, mixer_gain)
    channel = tp_index * local_width + jnp.arange(local_width, dtype=jnp.int32)
    windows = jnp.left_shift(jnp.full_like(channel, 2), channel // group_width)
    gathered = copy_for_each(normed_mixer, "tp").reshape(-1, model_width)
    projected = jnp.dot(gathered, proj_in, preferred_element_type=jnp.float32).astype(
        jnp.bfloat16
    )
    pooled = pool_mix(
        projected, pool_weight, pool_scale, windows, ep_index * projected.shape[0]
    )
    mixed_rows = sum_at_owner(
        jnp.dot(pooled, proj_out, preferred_element_type=jnp.float32).astype(jnp.bfloat16), "tp"
    ).astype(jnp.bfloat16)

    step = packet // chunks
    back = []
    for k in range(chunks):
        sent = outgoing[:, k * step : (k + 1) * step]
        arrived = same_core(sent, holders)
        rows = lax.all_gather(arrived, "tp", axis=0, tiled=False).reshape(-1, model_width)
        weight = weights[:, :, k * step : (k + 1) * step].reshape(-1, GROUP_SIZE)
        by_set = [
            lax.dynamic_slice_in_dim(
                weight, (place - s) % holders * local_experts, local_experts, 1
            )
            for s in range(holders)
        ]
        partial = expert_rows(rows, by_set, sets)
        summed = lax.psum_scatter(
            partial.reshape(tp_count, -1, model_width), "tp", scatter_dimension=0, tiled=True
        )
        back.append(same_core(summed.reshape(groups, step, model_width), holders))
    total = None
    pick_parts = pick.reshape(own_count, groups, packet)
    for k in range(chunks):
        part = jnp.dot(
            pick_parts[:, :, k * step : (k + 1) * step].reshape(own_count, -1),
            back[k].reshape(-1, model_width),
            preferred_element_type=jnp.float32,
        )
        total = part if total is None else total + part
    return (mixed_rows, total.astype(jnp.bfloat16))


def solution(mesh):
    return jax.shard_map(
        shards,
        mesh=mesh,
        in_specs=(
            P(("grp", "ep", "tp"), None),
            P(),
            P(None, "tp"),
            P("tp", None, None),
            P("tp"),
            P("tp", None),
            P(("grp", "ep", "tp"), None),
            P(),
            P(("grp", "ep"), None),
            P(("grp", "ep"), None),
            P("ep", None, "tp"),
            P("ep", None, "tp"),
            P("ep", "tp", None),
        ),
        out_specs=(P(("grp", "ep", "tp"), None), P(("grp", "ep", "tp"), None)),
        check_vma=False,
    )
```

```python
import jax
import jax.numpy as jnp
from jax import lax
from jax.experimental import pallas as pl
from jax.experimental.pallas import tpu as pltpu
from jax.sharding import PartitionSpec as P

GROUP_SIZE = 4

norm_eps = 1e-05
rim_rows = 15
chunks = 2
extra = 128


def shifted(value, axis, by):
    peers = lax.axis_size(axis)
    pairs = [(i, i + by) for i in range(peers) if 0 <= i + by < peers]
    return lax.ppermute(value, axis, pairs)


def turned(value, axis, by):
    peers = lax.axis_size(axis)
    return lax.ppermute(value, axis, [(i, (i + by) % peers) for i in range(peers)])


def tp_steps():
    peers = lax.axis_size("tp")
    steps = []
    for d in range(1, peers // 2 + 1):
        steps += [d] if 2 * d == peers else [d, -d]
    return steps


def spread(value):
    return [value] + [turned(value, "tp", s) for s in tp_steps()]


def collect(parts):
    arrived = [parts[0]] + [turned(p, "tp", -s) for p, s in zip(parts[1:], tp_steps())]
    total = arrived[0].astype(jnp.float32)
    for part in arrived[1:]:
        total = total + part.astype(jnp.float32)
    return total.astype(jnp.bfloat16)


def layer_norm(values, norm_gain):
    widened = values.astype(jnp.float32)
    center = jnp.mean(widened, axis=-1, keepdims=True)
    spread_of = jnp.mean(jnp.square(widened - center), axis=-1, keepdims=True)
    return ((widened - center) * lax.rsqrt(spread_of + norm_eps) * norm_gain).astype(jnp.bfloat16)


def pooled_diff(extended, windows, first_row):
    widened = extended.astype(jnp.float32)
    row_total = widened.shape[0] - rim_rows
    own_rows = widened[rim_rows:]
    window_sum = own_rows
    for offset in range(1, rim_rows + 1):
        lagged = widened[rim_rows - offset : rim_rows - offset + row_total]
        window_sum = window_sum + jnp.where(offset < windows[None, :], lagged, 0.0)
    position = first_row + jnp.arange(row_total, dtype=jnp.int32)
    covered = jnp.minimum(position[:, None] + 1, windows[None, :]).astype(jnp.float32)
    return (window_sum / covered - own_rows).astype(jnp.bfloat16)


def pool_mix(projected, pool_weight, pool_scale, windows, first_row):
    prior = shifted(projected[-rim_rows:], "ep", 1)
    differences = pooled_diff(jnp.concatenate([prior, projected], axis=0), windows, first_row)
    row_total, local_width = differences.shape
    grouped = differences.reshape(row_total, pool_weight.shape[0], pool_weight.shape[1])
    mixed_groups = jnp.einsum(
        "tgc,gcd->tgd", grouped, pool_weight, preferred_element_type=jnp.float32
    )
    return (mixed_groups.reshape(row_total, local_width) * pool_scale).astype(jnp.bfloat16)


def route_ranks(group, groups):
    rows = group.shape[0]
    named = group[:, None] == jnp.arange(groups, dtype=jnp.int32)
    order = jnp.arange(rows, dtype=jnp.int32)
    before = (order[:, None] > order[None, :]).astype(jnp.bfloat16)
    earlier = jnp.dot(before, named.astype(jnp.bfloat16), preferred_element_type=jnp.float32)
    return jnp.sum(jnp.where(named, earlier, 0.0), axis=1).astype(jnp.int32)


def same_core(value, holders):
    peers = lax.axis_size("ep")
    rings = [list(range(c, peers, holders)) for c in range(holders)]
    return lax.all_to_all(value, "ep", 0, 0, axis_index_groups=rings, tiled=True)


def expert_kernel(sources, holders, local_experts, width):
    def body(*refs):
        rows = refs[:sources]
        sets = [refs[sources + 3 * s : sources + 3 * s + 3] for s in range(holders)]
        outs = refs[sources + 3 * holders : 2 * sources + 3 * holders]
        joined, total = refs[2 * sources + 3 * holders :]
        step = pl.program_id(0)
        count = rows[0].shape[0]

        @pl.when(step == 0)
        def _():
            for b in range(sources):
                joined[b * count : (b + 1) * count] = rows[b][...]

        x = joined[:, :width]
        tail = joined[:, width:].astype(jnp.float32)
        lane = lax.broadcasted_iota(jnp.int32, tail.shape, 1)
        mine = (lane == step) | (lane == step + GROUP_SIZE)
        weight = jnp.sum(jnp.where(mine, tail, 0.0), axis=1, keepdims=True)

        for s in range(holders):
            gate, up, down = sets[s]

            @pl.when(step // local_experts == s)
            def _():
                gate_part = jnp.dot(x, gate[0], preferred_element_type=jnp.float32)
                up_part = jnp.dot(x, up[0], preferred_element_type=jnp.float32)
                hidden = (gate_part / (1.0 + jnp.exp(-gate_part)) * up_part * weight).astype(
                    jnp.bfloat16
                )
                part = jnp.dot(hidden, down[0], preferred_element_type=jnp.float32)

                @pl.when(step == 0)
                def _():
                    total[...] = part

                @pl.when(step > 0)
                def _():
                    total[...] += part

        @pl.when(step == holders * local_experts - 1)
        def _():
            for b in range(sources):
                outs[b][...] = total[b * count : (b + 1) * count].astype(jnp.bfloat16)

    return body


def expert_rows(rows, sets):
    sources = len(rows)
    holders = len(sets)
    local_experts, width, quarter = sets[0][0].shape
    count, full = rows[0].shape
    in_specs = [pl.BlockSpec((count, full), lambda i: (0, 0)) for _ in rows]
    for s in range(holders):
        low = s * local_experts

        def at(i, low=low):
            return (jnp.clip(i - low, 0, local_experts - 1), 0, 0)

        in_specs += [
            pl.BlockSpec((1, width, quarter), at),
            pl.BlockSpec((1, width, quarter), at),
            pl.BlockSpec((1, quarter, width), at),
        ]
    return pl.pallas_call(
        expert_kernel(sources, holders, local_experts, width),
        grid=(holders * local_experts,),
        in_specs=in_specs,
        out_specs=[pl.BlockSpec((count, width), lambda i: (0, 0)) for _ in rows],
        out_shape=[jax.ShapeDtypeStruct((count, width), jnp.bfloat16) for _ in rows],
        scratch_shapes=[
            pltpu.VMEM((sources * count, full), jnp.bfloat16),
            pltpu.VMEM((sources * count, width), jnp.float32),
        ],
        compiler_params=pltpu.CompilerParams(dimension_semantics=("arbitrary",)),
        cost_estimate=pl.CostEstimate(
            flops=6 * sources * count * width * quarter * holders * local_experts,
            bytes_accessed=6 * width * quarter * holders * local_experts
            + 2 * sources * count * (full + width),
            transcendentals=sources * count * quarter * holders * local_experts,
        ),
        name="experts",
    )(*rows, *[w for one in sets for w in one])


def shards(
    mixer_tokens,
    mixer_gain,
    proj_in,
    pool_weight,
    pool_scale,
    proj_out,
    expert_tokens,
    expert_gain,
    expert_route,
    route_gate,
    expert_gate,
    expert_up,
    expert_down,
):
    ep_count = lax.axis_size("ep")
    tp_index = lax.axis_index("tp")
    ep_index = lax.axis_index("ep")
    own_count, model_width = mixer_tokens.shape
    local_width = proj_in.shape[1]
    group_width = pool_weight.shape[1]
    local_experts = expert_gate.shape[0]
    experts = local_experts * ep_count
    capacity = own_count * GROUP_SIZE // experts
    packet = capacity * GROUP_SIZE // 2
    groups = experts // GROUP_SIZE
    holders = GROUP_SIZE // local_experts
    place = ep_index % holders
    step = packet // chunks

    own_start = tp_index * own_count
    own_route = lax.dynamic_slice_in_dim(expert_route, own_start, own_count, 0)
    own_gates = lax.dynamic_slice_in_dim(route_gate, own_start, own_count, 0)
    group = own_route[:, 0] // GROUP_SIZE
    rank = route_ranks(group, groups)
    slot = rank // step * (groups * step) + group * step + rank % step
    pick = (
        slot[:, None] == jnp.arange(chunks * groups * step, dtype=jnp.int32)
    ).astype(jnp.bfloat16)

    member = (own_route - place * local_experts) % GROUP_SIZE
    lane = jnp.arange(extra, dtype=jnp.int32)
    by_lane = jnp.zeros((own_count, extra), jnp.float32)
    for k in range(2):
        hit = lane[None, :] % GROUP_SIZE == member[:, k : k + 1]
        by_lane = by_lane + jnp.where(hit, own_gates[:, k : k + 1], 0.0)
    high = lax.reduce_precision(by_lane, 8, 7)
    tail = jnp.where(
        lane < GROUP_SIZE, high, jnp.where(lane < 2 * GROUP_SIZE, by_lane - high, 0.0)
    ).astype(jnp.bfloat16)

    normed_expert = layer_norm(expert_tokens, expert_gain)
    extended = jnp.concatenate([normed_expert, tail], axis=1)
    outgoing = []
    for k in range(chunks):
        part = jnp.einsum(
            "ts,td->sd",
            pick[:, k * groups * step : (k + 1) * groups * step],
            extended,
            preferred_element_type=jnp.float32,
        ).astype(jnp.bfloat16)
        outgoing.append(part.reshape(groups, step, model_width + extra))

    outgoing[0], mixer_tokens, expert_gate, expert_up, expert_down = lax.optimization_barrier(
        (outgoing[0], mixer_tokens, expert_gate, expert_up, expert_down)
    )
    own_set = (expert_gate, expert_up, expert_down)
    sets = [own_set]
    for s in range(1, holders):
        pairs = [(i, i - i % holders + (i - s) % holders) for i in range(ep_count)]
        sets.append(tuple(lax.ppermute(w, "ep", pairs) for w in own_set))

    normed_mixer = layer_norm(mixer_tokens, mixer_gain)
    channel = tp_index * local_width + jnp.arange(local_width, dtype=jnp.int32)
    windows = jnp.left_shift(jnp.full_like(channel, 2), channel // group_width)
    gathered = spread(normed_mixer)

    partials = []
    back = []
    for k in range(chunks):
        arrived = same_core(outgoing[k], holders).reshape(-1, model_width + extra)
        partials.append(expert_rows(spread(arrived), sets))
        summed = collect(partials[k])
        back.append(same_core(summed.reshape(groups, step, model_width), holders))

    tp_count = lax.axis_size("tp")
    stacked = jnp.stack(gathered)
    blocks = jnp.dot(
        stacked.reshape(-1, model_width), proj_in, preferred_element_type=jnp.float32
    ).astype(jnp.bfloat16)
    blocks = blocks.reshape(tp_count, own_count, local_width)
    source_step = {s % tp_count: r for r, s in enumerate([0] + tp_steps())}
    by_distance = jnp.stack([blocks[source_step[d]] for d in range(tp_count)])
    order = (tp_index - jnp.arange(tp_count, dtype=jnp.int32)) % tp_count
    projected = by_distance[order].reshape(-1, local_width)
    pooled = pool_mix(
        projected, pool_weight, pool_scale, windows, ep_index * projected.shape[0]
    )
    product = jnp.dot(pooled, proj_out, preferred_element_type=jnp.float32).astype(jnp.bfloat16)
    product = product.reshape(tp_count, own_count, model_width)
    parts = [
        lax.dynamic_index_in_dim(product, (tp_index - s) % tp_count, 0, keepdims=False)
        for s in [0] + tp_steps()
    ]
    parts, _ = lax.optimization_barrier((parts, partials[-1][0]))
    mixed_rows = collect(parts)

    total = None
    for k in range(chunks):
        part = jnp.dot(
            pick[:, k * groups * step : (k + 1) * groups * step],
            back[k].reshape(-1, model_width),
            preferred_element_type=jnp.float32,
        )
        total = part if total is None else total + part
    return (mixed_rows, total.astype(jnp.bfloat16))


def solution(mesh):
    return jax.shard_map(
        shards,
        mesh=mesh,
        in_specs=(
            P(("grp", "ep", "tp"), None),
            P(),
            P(None, "tp"),
            P("tp", None, None),
            P("tp"),
            P("tp", None),
            P(("grp", "ep", "tp"), None),
            P(),
            P(("grp", "ep"), None),
            P(("grp", "ep"), None),
            P("ep", None, "tp"),
            P("ep", None, "tp"),
            P("ep", "tp", None),
        ),
        out_specs=(P(("grp", "ep", "tp"), None), P(("grp", "ep", "tp"), None)),
        check_vma=False,
    )
```

```python
import jax
import jax.numpy as jnp
from jax import lax
from jax.experimental import pallas as pl
from jax.experimental.pallas import tpu as pltpu
from jax.sharding import PartitionSpec as P


GROUP_SIZE = 4

norm_eps = 1e-05
rim_rows = 15
chunks = 2
extra = 128
lift_block = 256
lower_block = 128


def shifted(value, axis, by):
    peers = lax.axis_size(axis)
    pairs = [(i, i + by) for i in range(peers) if 0 <= i + by < peers]
    return lax.ppermute(value, axis, pairs)


def turned(value, axis, by):
    peers = lax.axis_size(axis)
    return lax.ppermute(value, axis, [(i, (i + by) % peers) for i in range(peers)])


def tp_steps():
    peers = lax.axis_size("tp")
    steps = []
    for d in range(1, peers // 2 + 1):
        steps += [d] if 2 * d == peers else [d, -d]
    return steps


def spread(value):
    return [value] + [turned(value, "tp", s) for s in tp_steps()]


def collect(parts):
    arrived = [parts[0]] + [turned(p, "tp", -s) for p, s in zip(parts[1:], tp_steps())]
    total = arrived[0].astype(jnp.float32)
    for part in arrived[1:]:
        total = total + part.astype(jnp.float32)
    return total.astype(jnp.bfloat16)


def layer_norm(values, norm_gain):
    widened = values.astype(jnp.float32)
    center = jnp.mean(widened, axis=-1, keepdims=True)
    spread_of = jnp.mean(jnp.square(widened - center), axis=-1, keepdims=True)
    return ((widened - center) * lax.rsqrt(spread_of + norm_eps) * norm_gain).astype(jnp.bfloat16)


def pooled_diff(extended, windows, first_row):
    widened = extended.astype(jnp.float32)
    row_total = widened.shape[0] - rim_rows
    own_rows = widened[rim_rows:]
    window_sum = own_rows
    for offset in range(1, rim_rows + 1):
        lagged = widened[rim_rows - offset : rim_rows - offset + row_total]
        window_sum = window_sum + jnp.where(offset < windows[None, :], lagged, 0.0)
    position = first_row + jnp.arange(row_total, dtype=jnp.int32)
    covered = jnp.minimum(position[:, None] + 1, windows[None, :]).astype(jnp.float32)
    return (window_sum / covered - own_rows).astype(jnp.bfloat16)


def pool_mix(projected, pool_weight, pool_scale, windows, first_row):
    prior = shifted(projected[-rim_rows:], "ep", 1)
    differences = pooled_diff(jnp.concatenate([prior, projected], axis=0), windows, first_row)
    row_total, local_width = differences.shape
    grouped = differences.reshape(row_total, pool_weight.shape[0], pool_weight.shape[1])
    mixed_groups = jnp.einsum(
        "tgc,gcd->tgd", grouped, pool_weight, preferred_element_type=jnp.float32
    )
    return (mixed_groups.reshape(row_total, local_width) * pool_scale).astype(jnp.bfloat16)


def route_ranks(group, groups):
    rows = group.shape[0]
    named = group[:, None] == jnp.arange(groups, dtype=jnp.int32)
    order = jnp.arange(rows, dtype=jnp.int32)
    before = (order[:, None] > order[None, :]).astype(jnp.bfloat16)
    earlier = jnp.dot(before, named.astype(jnp.bfloat16), preferred_element_type=jnp.float32)
    return jnp.sum(jnp.where(named, earlier, 0.0), axis=1).astype(jnp.int32)


def same_core(value, holders):
    peers = lax.axis_size("ep")
    rings = [list(range(c, peers, holders)) for c in range(holders)]
    return lax.all_to_all(value, "ep", 0, 0, axis_index_groups=rings, tiled=True)


def ring_gather(value):
    half = value.shape[0] // 2
    before = turned(value, "tp", 1)
    after = turned(value, "tp", -1)
    low = turned(before[:half], "tp", 1)
    high = turned(after[half:], "tp", -1)
    return [value, before, after, low, high]


def add_halves(own, lows, highs):
    half = lows[0].shape[0]

    def body(own_ref, *refs):
        out = refs[-1]
        for k, group in enumerate([refs[: len(lows)], refs[len(lows) : -1]]):
            rows = pl.ds(k * half, half)
            total = own_ref[rows].astype(jnp.float32)
            for ref in group:
                total = total + ref[...].astype(jnp.float32)
            out[rows] = total.astype(jnp.bfloat16)

    return pl.pallas_call(
        body, out_shape=jax.ShapeDtypeStruct(own.shape, jnp.bfloat16), name="add_halves"
    )(own, *lows, *highs)


def ring_sum(own, before_low, before_high, after_low, after_high, low, high):
    def joined(x, y):
        return (x.astype(jnp.float32) + y.astype(jnp.float32)).astype(jnp.bfloat16)

    low = turned(low, "tp", 1)
    high = turned(high, "tp", -1)
    after_high = turned(after_high, "tp", 1)
    before_low = turned(before_low, "tp", -1)
    after_low = turned(joined(after_low, low), "tp", 1)
    before_high = turned(joined(before_high, high), "tp", -1)
    return add_halves(own, [after_low, before_low], [after_high, before_high])


def expert_kernel(in_counts, out_counts, holders, local_experts, width, quarter):
    experts = holders * local_experts

    def body(*refs):
        ins, rest = refs[: len(in_counts)], refs[len(in_counts) :]
        weights, rest = rest[: 3 * holders], rest[3 * holders :]
        outs, rest = rest[: len(out_counts)], rest[len(out_counts) :]
        joined, both, downs, hidden, result, in_sem, up_sem, down_sem, out_sem = rest

        def row_copies(refs, counts, make):
            start = 0
            copies = []
            for k, count in enumerate(counts):
                copies.append(make(refs[k], start, count, k))
                start += count
            return copies

        entering = row_copies(
            ins,
            in_counts,
            lambda ref, start, count, k: pltpu.make_async_copy(
                ref, joined.at[pl.ds(start, count)], in_sem.at[k]
            ),
        )
        leaving = row_copies(
            outs,
            out_counts,
            lambda ref, start, count, k: pltpu.make_async_copy(
                result.at[pl.ds(start, count)], ref, out_sem.at[k]
            ),
        )
        lifts, lowers = [], []
        for e in range(experts):
            gate, up, down = weights[3 * (e // local_experts) : 3 * (e // local_experts) + 3]
            i = e % local_experts
            lifts.append(
                pltpu.make_async_copy(gate.at[i], both.at[e, :, pl.ds(0, quarter)], up_sem.at[0, e])
            )
            lifts.append(
                pltpu.make_async_copy(
                    up.at[i], both.at[e, :, pl.ds(quarter, quarter)], up_sem.at[1, e]
                )
            )
            lowers.append(pltpu.make_async_copy(down.at[i], downs.at[e], down_sem.at[e]))
        for copy in lifts[:2] + entering + lifts[2:] + lowers:
            copy.start()
        for copy in entering:
            copy.wait()

        def lift(e, carry):
            for k in range(2):
                part = both.at[e, :, pl.ds(k * quarter, quarter)]
                pltpu.make_async_copy(part, part, up_sem.at[k, e]).wait()

            def lift_rows(i, carry):
                rows = pl.ds(pl.multiple_of(i * lift_block, lift_block), lift_block)
                tail = joined[rows, width:].astype(jnp.float32)
                lane = lax.broadcasted_iota(jnp.int32, tail.shape, 1)
                mine = (lane == e) | (lane == e + GROUP_SIZE)
                weight = jnp.sum(jnp.where(mine, tail, 0.0), axis=1, keepdims=True)
                parts = jnp.dot(
                    joined[rows, :width], both[e], preferred_element_type=jnp.float32
                )
                gate_part = parts[:, :quarter]
                hidden[e, rows] = (
                    gate_part / (1.0 + jnp.exp(-gate_part)) * (parts[:, quarter:] * weight)
                ).astype(jnp.bfloat16)
                return carry

            return lax.fori_loop(0, joined.shape[0] // lift_block, lift_rows, carry)

        lax.fori_loop(0, experts, lift, 0)
        for copy in lowers:
            copy.wait()

        def lower(i, carry):
            rows = pl.ds(pl.multiple_of(i * lower_block, lower_block), lower_block)
            grouped = jnp.concatenate([hidden[e, rows] for e in range(experts)], axis=1)
            total = jnp.dot(
                grouped,
                downs[...].reshape(experts * quarter, width),
                preferred_element_type=jnp.float32,
            )
            result[rows] = total.astype(jnp.bfloat16)
            return carry

        lax.fori_loop(0, joined.shape[0] // lower_block, lower, 0)
        for copy in leaving:
            copy.start()
        for copy in leaving:
            copy.wait()

    return body


def expert_rows(rows, out_counts, sets):
    holders = len(sets)
    local_experts, width, quarter = sets[0][0].shape
    experts = holders * local_experts
    in_counts = [r.shape[0] for r in rows]
    total = sum(in_counts)
    full = rows[0].shape[1]
    anywhere = pl.BlockSpec(memory_space=pl.ANY)
    return pl.pallas_call(
        expert_kernel(in_counts, out_counts, holders, local_experts, width, quarter),
        in_specs=[anywhere] * (len(rows) + 3 * holders),
        out_specs=[anywhere] * len(out_counts),
        out_shape=[jax.ShapeDtypeStruct((count, width), jnp.bfloat16) for count in out_counts],
        scratch_shapes=[
            pltpu.VMEM((total, full), jnp.bfloat16),
            pltpu.VMEM((experts, width, 2 * quarter), jnp.bfloat16),
            pltpu.VMEM((experts, quarter, width), jnp.bfloat16),
            pltpu.VMEM((experts, total, quarter), jnp.bfloat16),
            pltpu.VMEM((total, width), jnp.bfloat16),
            pltpu.SemaphoreType.DMA((len(in_counts),)),
            pltpu.SemaphoreType.DMA((2, experts)),
            pltpu.SemaphoreType.DMA((experts,)),
            pltpu.SemaphoreType.DMA((len(out_counts),)),
        ],
        cost_estimate=pl.CostEstimate(
            flops=6 * total * width * quarter * experts,
            bytes_accessed=6 * width * quarter * experts + 2 * total * (full + width),
            transcendentals=total * quarter * experts,
        ),
        name="experts",
    )(*rows, *[w for one in sets for w in one])


def layer(
    mixer_tokens,
    mixer_gain,
    proj_in,
    pool_weight,
    pool_scale,
    proj_out,
    expert_tokens,
    expert_gain,
    expert_route,
    route_gate,
    expert_gate,
    expert_up,
    expert_down,
):
    ep_count = lax.axis_size("ep")
    tp_index = lax.axis_index("tp")
    ep_index = lax.axis_index("ep")
    own_count, model_width = mixer_tokens.shape
    local_width = proj_in.shape[1]
    group_width = pool_weight.shape[1]
    local_experts = expert_gate.shape[0]
    experts = local_experts * ep_count
    capacity = own_count * GROUP_SIZE // experts
    packet = capacity * GROUP_SIZE // 2
    groups = experts // GROUP_SIZE
    holders = GROUP_SIZE // local_experts
    place = ep_index % holders
    step = packet // chunks

    own_start = tp_index * own_count
    own_route = lax.dynamic_slice_in_dim(expert_route, own_start, own_count, 0)
    own_gates = lax.dynamic_slice_in_dim(route_gate, own_start, own_count, 0)
    group = own_route[:, 0] // GROUP_SIZE
    rank = route_ranks(group, groups)
    slot = rank // step * (groups * step) + group * step + rank % step
    pick = (
        slot[:, None] == jnp.arange(chunks * groups * step, dtype=jnp.int32)
    ).astype(jnp.bfloat16)

    member = (own_route - place * local_experts) % GROUP_SIZE
    lane = jnp.arange(extra, dtype=jnp.int32)
    by_lane = jnp.zeros((own_count, extra), jnp.float32)
    for k in range(2):
        hit = lane[None, :] % GROUP_SIZE == member[:, k : k + 1]
        by_lane = by_lane + jnp.where(hit, own_gates[:, k : k + 1], 0.0)
    high = lax.reduce_precision(by_lane, 8, 7)
    tail = jnp.where(
        lane < GROUP_SIZE, high, jnp.where(lane < 2 * GROUP_SIZE, by_lane - high, 0.0)
    ).astype(jnp.bfloat16)

    normed_expert = layer_norm(expert_tokens, expert_gain)
    extended = jnp.concatenate([normed_expert, tail], axis=1)
    outgoing = []
    for k in range(chunks):
        part = jnp.einsum(
            "ts,td->sd",
            pick[:, k * groups * step : (k + 1) * groups * step],
            extended,
            preferred_element_type=jnp.float32,
        ).astype(jnp.bfloat16)
        outgoing.append(part.reshape(groups, step, model_width + extra))

    outgoing[0], mixer_tokens, expert_gate, expert_up, expert_down = lax.optimization_barrier(
        (outgoing[0], mixer_tokens, expert_gate, expert_up, expert_down)
    )
    own_set = (expert_gate, expert_up, expert_down)
    sets = [own_set]
    for s in range(1, holders):
        pairs = [(i, i - i % holders + (i - s) % holders) for i in range(ep_count)]
        sets.append(tuple(lax.ppermute(w, "ep", pairs) for w in own_set))

    normed_mixer = layer_norm(mixer_tokens, mixer_gain)
    channel = tp_index * local_width + jnp.arange(local_width, dtype=jnp.int32)
    windows = jnp.left_shift(jnp.full_like(channel, 2), channel // group_width)
    gathered = spread(normed_mixer)

    partials = []
    back = []
    for k in range(chunks):
        arrived = same_core(outgoing[k], holders).reshape(-1, model_width + extra)
        rows = ring_gather(arrived)
        count = arrived.shape[0]
        half = count // 2
        partials.append(expert_rows(rows, [count] + [half] * 6, sets))
        summed = ring_sum(*partials[k])
        back.append(same_core(summed.reshape(groups, step, model_width), holders))

    tp_count = lax.axis_size("tp")
    stacked = jnp.stack(gathered)
    blocks = jnp.dot(
        stacked.reshape(-1, model_width), proj_in, preferred_element_type=jnp.float32
    ).astype(jnp.bfloat16)
    blocks = blocks.reshape(tp_count, own_count, local_width)
    source_step = {s % tp_count: r for r, s in enumerate([0] + tp_steps())}
    by_distance = jnp.stack([blocks[source_step[d]] for d in range(tp_count)])
    order = (tp_index - jnp.arange(tp_count, dtype=jnp.int32)) % tp_count
    projected = by_distance[order].reshape(-1, local_width)
    pooled = pool_mix(
        projected, pool_weight, pool_scale, windows, ep_index * projected.shape[0]
    )
    product = jnp.dot(pooled, proj_out, preferred_element_type=jnp.float32).astype(jnp.bfloat16)
    product = product.reshape(tp_count, own_count, model_width)
    parts = [
        lax.dynamic_index_in_dim(product, (tp_index - s) % tp_count, 0, keepdims=False)
        for s in [0] + tp_steps()
    ]
    parts, _ = lax.optimization_barrier((parts, partials[-1][0]))
    mixed_rows = collect(parts)

    total = None
    for k in range(chunks):
        part = jnp.dot(
            pick[:, k * groups * step : (k + 1) * groups * step],
            back[k].reshape(-1, model_width),
            preferred_element_type=jnp.float32,
        )
        total = part if total is None else total + part
    return (mixed_rows, total.astype(jnp.bfloat16))


def solution(mesh):
    return jax.shard_map(
        layer,
        mesh=mesh,
        in_specs=(
            P(("grp", "ep", "tp"), None),
            P(),
            P(None, "tp"),
            P("tp", None, None),
            P("tp"),
            P("tp", None),
            P(("grp", "ep", "tp"), None),
            P(),
            P(("grp", "ep"), None),
            P(("grp", "ep"), None),
            P("ep", None, "tp"),
            P("ep", None, "tp"),
            P("ep", "tp", None),
        ),
        out_specs=(P(("grp", "ep", "tp"), None), P(("grp", "ep", "tp"), None)),
        check_vma=False,
    )
```

```python
import jax
import jax.numpy as jnp
from jax import lax
from jax.experimental import pallas as pl
from jax.experimental.pallas import tpu as pltpu
from jax.sharding import PartitionSpec as P


GROUP_SIZE = 4

norm_eps = 1e-05
rim_rows = 15
chunks = 2
extra = 128
lift_block = 256
lower_block = 128


def shifted(value, axis, by):
    peers = lax.axis_size(axis)
    pairs = [(i, i + by) for i in range(peers) if 0 <= i + by < peers]
    return lax.ppermute(value, axis, pairs)


def turned(value, axis, by):
    peers = lax.axis_size(axis)
    return lax.ppermute(value, axis, [(i, (i + by) % peers) for i in range(peers)])


def tp_steps():
    peers = lax.axis_size("tp")
    steps = []
    for d in range(1, peers // 2 + 1):
        steps += [d] if 2 * d == peers else [d, -d]
    return steps


def spread(value):
    return [value] + [turned(value, "tp", s) for s in tp_steps()]


def collect(parts):
    arrived = [parts[0]] + [turned(p, "tp", -s) for p, s in zip(parts[1:], tp_steps())]
    total = arrived[0].astype(jnp.float32)
    for part in arrived[1:]:
        total = total + part.astype(jnp.float32)
    return total.astype(jnp.bfloat16)


def layer_norm(values, norm_gain):
    widened = values.astype(jnp.float32)
    center = jnp.mean(widened, axis=-1, keepdims=True)
    spread_of = jnp.mean(jnp.square(widened - center), axis=-1, keepdims=True)
    return ((widened - center) * lax.rsqrt(spread_of + norm_eps) * norm_gain).astype(jnp.bfloat16)


def pooled_diff(extended, windows, first_row):
    widened = extended.astype(jnp.float32)
    row_total = widened.shape[0] - rim_rows
    own_rows = widened[rim_rows:]
    window_sum = own_rows
    for offset in range(1, rim_rows + 1):
        lagged = widened[rim_rows - offset : rim_rows - offset + row_total]
        window_sum = window_sum + jnp.where(offset < windows[None, :], lagged, 0.0)
    position = first_row + jnp.arange(row_total, dtype=jnp.int32)
    covered = jnp.minimum(position[:, None] + 1, windows[None, :]).astype(jnp.float32)
    return (window_sum / covered - own_rows).astype(jnp.bfloat16)


def pool_mix(projected, pool_weight, pool_scale, windows, first_row):
    prior = shifted(projected[-rim_rows:], "ep", 1)
    differences = pooled_diff(jnp.concatenate([prior, projected], axis=0), windows, first_row)
    row_total, local_width = differences.shape
    grouped = differences.reshape(row_total, pool_weight.shape[0], pool_weight.shape[1])
    mixed_groups = jnp.einsum(
        "tgc,gcd->tgd", grouped, pool_weight, preferred_element_type=jnp.float32
    )
    return (mixed_groups.reshape(row_total, local_width) * pool_scale).astype(jnp.bfloat16)


def route_ranks(group, groups):
    rows = group.shape[0]
    named = group[:, None] == jnp.arange(groups, dtype=jnp.int32)
    order = jnp.arange(rows, dtype=jnp.int32)
    before = (order[:, None] > order[None, :]).astype(jnp.bfloat16)
    earlier = jnp.dot(before, named.astype(jnp.bfloat16), preferred_element_type=jnp.float32)
    return jnp.sum(jnp.where(named, earlier, 0.0), axis=1).astype(jnp.int32)


def same_core(value, holders):
    peers = lax.axis_size("ep")
    rings = [list(range(c, peers, holders)) for c in range(holders)]
    return lax.all_to_all(value, "ep", 0, 0, axis_index_groups=rings, tiled=True)


def ring_gather(value):
    half = value.shape[0] // 2
    before = turned(value, "tp", 1)
    after = turned(value, "tp", -1)
    low = turned(before[:half], "tp", 1)
    high = turned(after[half:], "tp", -1)
    return [value, before, after, low, high]


def add_halves(own, lows, highs):
    half = lows[0].shape[0]

    def body(own_ref, *refs):
        out = refs[-1]
        for k, group in enumerate([refs[: len(lows)], refs[len(lows) : -1]]):
            rows = pl.ds(k * half, half)
            total = own_ref[rows].astype(jnp.float32)
            for ref in group:
                total = total + ref[...].astype(jnp.float32)
            out[rows] = total.astype(jnp.bfloat16)

    return pl.pallas_call(
        body, out_shape=jax.ShapeDtypeStruct(own.shape, jnp.bfloat16), name="add_halves"
    )(own, *lows, *highs)


def ring_sum(own, before_low, before_high, after_low, after_high, low, high):
    def joined(x, y):
        return (x.astype(jnp.float32) + y.astype(jnp.float32)).astype(jnp.bfloat16)

    low = turned(low, "tp", 1)
    high = turned(high, "tp", -1)
    after_high = turned(after_high, "tp", 1)
    before_low = turned(before_low, "tp", -1)
    after_low = turned(joined(after_low, low), "tp", 1)
    before_high = turned(joined(before_high, high), "tp", -1)
    return add_halves(own, [after_low, before_low], [after_high, before_high])


def expert_kernel(in_counts, out_counts, holders, local_experts, width, quarter):
    experts = holders * local_experts

    def body(*refs):
        ins, rest = refs[: len(in_counts)], refs[len(in_counts) :]
        weights, rest = rest[: 3 * holders], rest[3 * holders :]
        outs, rest = rest[: len(out_counts)], rest[len(out_counts) :]
        joined, both, downs, hidden, result, in_sem, up_sem, down_sem, out_sem = rest

        def row_copies(refs, counts, make):
            start = 0
            copies = []
            for k, count in enumerate(counts):
                copies.append(make(refs[k], start, count, k))
                start += count
            return copies

        entering = row_copies(
            ins,
            in_counts,
            lambda ref, start, count, k: pltpu.make_async_copy(
                ref, joined.at[pl.ds(start, count)], in_sem.at[k]
            ),
        )
        leaving = row_copies(
            outs,
            out_counts,
            lambda ref, start, count, k: pltpu.make_async_copy(
                result.at[pl.ds(start, count)], ref, out_sem.at[k]
            ),
        )
        lifts, lowers = [], []
        for e in range(experts):
            gate, up, down = weights[3 * (e // local_experts) : 3 * (e // local_experts) + 3]
            i = e % local_experts
            lifts.append(
                pltpu.make_async_copy(gate.at[i], both.at[e, :, pl.ds(0, quarter)], up_sem.at[0, e])
            )
            lifts.append(
                pltpu.make_async_copy(
                    up.at[i], both.at[e, :, pl.ds(quarter, quarter)], up_sem.at[1, e]
                )
            )
            lowers.append(pltpu.make_async_copy(down.at[i], downs.at[e], down_sem.at[e]))
        for copy in lifts[:2] + entering + lifts[2:] + lowers:
            copy.start()
        for copy in entering:
            copy.wait()

        def lift(e, carry):
            for k in range(2):
                part = both.at[e, :, pl.ds(k * quarter, quarter)]
                pltpu.make_async_copy(part, part, up_sem.at[k, e]).wait()

            def lift_rows(i, carry):
                rows = pl.ds(pl.multiple_of(i * lift_block, lift_block), lift_block)
                tail = joined[rows, width:].astype(jnp.float32)
                lane = lax.broadcasted_iota(jnp.int32, tail.shape, 1)
                mine = (lane == e) | (lane == e + GROUP_SIZE)
                weight = jnp.sum(jnp.where(mine, tail, 0.0), axis=1, keepdims=True)
                parts = jnp.dot(
                    joined[rows, :width], both[e], preferred_element_type=jnp.float32
                )
                gate_part = parts[:, :quarter]
                hidden[e, rows] = (
                    gate_part / (1.0 + jnp.exp(-gate_part)) * (parts[:, quarter:] * weight)
                ).astype(jnp.bfloat16)
                return carry

            return lax.fori_loop(0, joined.shape[0] // lift_block, lift_rows, carry)

        lax.fori_loop(0, experts, lift, 0)
        for copy in lowers:
            copy.wait()

        def lower(i, carry):
            rows = pl.ds(pl.multiple_of(i * lower_block, lower_block), lower_block)
            grouped = jnp.concatenate([hidden[e, rows] for e in range(experts)], axis=1)
            total = jnp.dot(
                grouped,
                downs[...].reshape(experts * quarter, width),
                preferred_element_type=jnp.float32,
            )
            result[rows] = total.astype(jnp.bfloat16)
            return carry

        lax.fori_loop(0, joined.shape[0] // lower_block, lower, 0)
        for copy in leaving:
            copy.start()
        for copy in leaving:
            copy.wait()

    return body


def expert_rows(rows, out_counts, sets):
    holders = len(sets)
    local_experts, width, quarter = sets[0][0].shape
    experts = holders * local_experts
    in_counts = [r.shape[0] for r in rows]
    total = sum(in_counts)
    full = rows[0].shape[1]
    anywhere = pl.BlockSpec(memory_space=pl.ANY)
    return pl.pallas_call(
        expert_kernel(in_counts, out_counts, holders, local_experts, width, quarter),
        in_specs=[anywhere] * (len(rows) + 3 * holders),
        out_specs=[anywhere] * len(out_counts),
        out_shape=[jax.ShapeDtypeStruct((count, width), jnp.bfloat16) for count in out_counts],
        scratch_shapes=[
            pltpu.VMEM((total, full), jnp.bfloat16),
            pltpu.VMEM((experts, width, 2 * quarter), jnp.bfloat16),
            pltpu.VMEM((experts, quarter, width), jnp.bfloat16),
            pltpu.VMEM((experts, total, quarter), jnp.bfloat16),
            pltpu.VMEM((total, width), jnp.bfloat16),
            pltpu.SemaphoreType.DMA((len(in_counts),)),
            pltpu.SemaphoreType.DMA((2, experts)),
            pltpu.SemaphoreType.DMA((experts,)),
            pltpu.SemaphoreType.DMA((len(out_counts),)),
        ],
        cost_estimate=pl.CostEstimate(
            flops=6 * total * width * quarter * experts,
            bytes_accessed=6 * width * quarter * experts + 2 * total * (full + width),
            transcendentals=total * quarter * experts,
        ),
        name="experts",
    )(*rows, *[w for one in sets for w in one])


def layer(
    mixer_tokens,
    mixer_gain,
    proj_in,
    pool_weight,
    pool_scale,
    proj_out,
    expert_tokens,
    expert_gain,
    expert_route,
    route_gate,
    expert_gate,
    expert_up,
    expert_down,
):
    ep_count = lax.axis_size("ep")
    tp_index = lax.axis_index("tp")
    ep_index = lax.axis_index("ep")
    own_count, model_width = mixer_tokens.shape
    local_width = proj_in.shape[1]
    group_width = pool_weight.shape[1]
    local_experts = expert_gate.shape[0]
    experts = local_experts * ep_count
    capacity = own_count * GROUP_SIZE // experts
    packet = capacity * GROUP_SIZE // 2
    groups = experts // GROUP_SIZE
    holders = GROUP_SIZE // local_experts
    place = ep_index % holders
    step = packet // chunks

    own_start = tp_index * own_count
    own_route = lax.dynamic_slice_in_dim(expert_route, own_start, own_count, 0)
    own_gates = lax.dynamic_slice_in_dim(route_gate, own_start, own_count, 0)
    group = own_route[:, 0] // GROUP_SIZE
    rank = route_ranks(group, groups)
    slot = rank // step * (groups * step) + group * step + rank % step
    pick = (
        slot[:, None] == jnp.arange(chunks * groups * step, dtype=jnp.int32)
    ).astype(jnp.bfloat16)

    member = (own_route - place * local_experts) % GROUP_SIZE
    lane = jnp.arange(extra, dtype=jnp.int32)
    by_lane = jnp.zeros((own_count, extra), jnp.float32)
    for k in range(2):
        hit = lane[None, :] % GROUP_SIZE == member[:, k : k + 1]
        by_lane = by_lane + jnp.where(hit, own_gates[:, k : k + 1], 0.0)
    high = lax.reduce_precision(by_lane, 8, 7)
    tail = jnp.where(
        lane < GROUP_SIZE, high, jnp.where(lane < 2 * GROUP_SIZE, by_lane - high, 0.0)
    ).astype(jnp.bfloat16)

    normed_expert = layer_norm(expert_tokens, expert_gain)
    extended = jnp.concatenate([normed_expert, tail], axis=1)
    outgoing = []
    for k in range(chunks):
        part = jnp.einsum(
            "ts,td->sd",
            pick[:, k * groups * step : (k + 1) * groups * step],
            extended,
            preferred_element_type=jnp.float32,
        ).astype(jnp.bfloat16)
        outgoing.append(part.reshape(groups, step, model_width + extra))

    outgoing[0], mixer_tokens, expert_gate, expert_up, expert_down = lax.optimization_barrier(
        (outgoing[0], mixer_tokens, expert_gate, expert_up, expert_down)
    )
    own_set = (expert_gate, expert_up, expert_down)
    sets = [own_set]
    for s in range(1, holders):
        pairs = [(i, i - i % holders + (i - s) % holders) for i in range(ep_count)]
        sets.append(tuple(lax.ppermute(w, "ep", pairs) for w in own_set))

    normed_mixer = layer_norm(mixer_tokens, mixer_gain)
    channel = tp_index * local_width + jnp.arange(local_width, dtype=jnp.int32)
    windows = jnp.left_shift(jnp.full_like(channel, 2), channel // group_width)
    gathered = spread(normed_mixer)

    partials = []
    back = []
    for k in range(chunks):
        arrived = same_core(outgoing[k], holders).reshape(-1, model_width + extra)
        rows = ring_gather(arrived) if k + 1 < chunks else spread(arrived)
        count = arrived.shape[0]
        half = count // 2
        partials.append(expert_rows(rows, [count] + [half] * 6, sets))
        summed = ring_sum(*partials[k])
        back.append(same_core(summed.reshape(groups, step, model_width), holders))

    tp_count = lax.axis_size("tp")
    stacked = jnp.stack(gathered)
    blocks = jnp.dot(
        stacked.reshape(-1, model_width), proj_in, preferred_element_type=jnp.float32
    ).astype(jnp.bfloat16)
    blocks = blocks.reshape(tp_count, own_count, local_width)
    source_step = {s % tp_count: r for r, s in enumerate([0] + tp_steps())}
    by_distance = jnp.stack([blocks[source_step[d]] for d in range(tp_count)])
    order = (tp_index - jnp.arange(tp_count, dtype=jnp.int32)) % tp_count
    projected = by_distance[order].reshape(-1, local_width)
    pooled = pool_mix(
        projected, pool_weight, pool_scale, windows, ep_index * projected.shape[0]
    )
    product = jnp.dot(pooled, proj_out, preferred_element_type=jnp.float32).astype(
        jnp.bfloat16
    )
    product = product.reshape(tp_count, own_count, model_width)
    parts = [
        lax.dynamic_index_in_dim(product, (tp_index - s) % tp_count, 0, keepdims=False)
        for s in [0] + tp_steps()
    ]
    mixed_rows = collect(parts)

    total = None
    for k in range(chunks):
        part = jnp.dot(
            pick[:, k * groups * step : (k + 1) * groups * step],
            back[k].reshape(-1, model_width),
            preferred_element_type=jnp.float32,
        )
        total = part if total is None else total + part
    return (mixed_rows, total.astype(jnp.bfloat16))


def solution(mesh):
    return jax.shard_map(
        layer,
        mesh=mesh,
        in_specs=(
            P(("grp", "ep", "tp"), None),
            P(),
            P(None, "tp"),
            P("tp", None, None),
            P("tp"),
            P("tp", None),
            P(("grp", "ep", "tp"), None),
            P(),
            P(("grp", "ep"), None),
            P(("grp", "ep"), None),
            P("ep", None, "tp"),
            P("ep", None, "tp"),
            P("ep", "tp", None),
        ),
        out_specs=(P(("grp", "ep", "tp"), None), P(("grp", "ep", "tp"), None)),
        check_vma=False,
    )
```

```python
import jax
import jax.numpy as jnp
from jax import lax
from jax.experimental import pallas as pl
from jax.experimental.pallas import tpu as pltpu
from jax.sharding import PartitionSpec as P


GROUP_SIZE = 4

norm_eps = 1e-05
rim_rows = 15
chunks = 2
extra = 128
lift_block = 256
lower_block = 128


def shifted(value, axis, by):
    peers = lax.axis_size(axis)
    pairs = [(i, i + by) for i in range(peers) if 0 <= i + by < peers]
    return lax.ppermute(value, axis, pairs)


def turned(value, axis, by):
    peers = lax.axis_size(axis)
    return lax.ppermute(value, axis, [(i, (i + by) % peers) for i in range(peers)])


def tp_steps():
    peers = lax.axis_size("tp")
    steps = []
    for d in range(1, peers // 2 + 1):
        steps += [d] if 2 * d == peers else [d, -d]
    return steps


def spread(value):
    return [value] + [turned(value, "tp", s) for s in tp_steps()]


def collect(parts):
    arrived = [parts[0]] + [turned(p, "tp", -s) for p, s in zip(parts[1:], tp_steps())]
    total = arrived[0].astype(jnp.float32)
    for part in arrived[1:]:
        total = total + part.astype(jnp.float32)
    return total.astype(jnp.bfloat16)


def layer_norm(values, norm_gain):
    widened = values.astype(jnp.float32)
    center = jnp.mean(widened, axis=-1, keepdims=True)
    spread_of = jnp.mean(jnp.square(widened - center), axis=-1, keepdims=True)
    return ((widened - center) * lax.rsqrt(spread_of + norm_eps) * norm_gain).astype(jnp.bfloat16)


def pooled_diff(extended, windows, first_row):
    widened = extended.astype(jnp.float32)
    row_total = widened.shape[0] - rim_rows
    own_rows = widened[rim_rows:]
    window_sum = own_rows
    for offset in range(1, rim_rows + 1):
        lagged = widened[rim_rows - offset : rim_rows - offset + row_total]
        window_sum = window_sum + jnp.where(offset < windows[None, :], lagged, 0.0)
    position = first_row + jnp.arange(row_total, dtype=jnp.int32)
    covered = jnp.minimum(position[:, None] + 1, windows[None, :]).astype(jnp.float32)
    return (window_sum / covered - own_rows).astype(jnp.bfloat16)


def pool_mix(projected, pool_weight, pool_scale, windows, first_row):
    prior = shifted(projected[-rim_rows:], "ep", 1)
    differences = pooled_diff(jnp.concatenate([prior, projected], axis=0), windows, first_row)
    row_total, local_width = differences.shape
    grouped = differences.reshape(row_total, pool_weight.shape[0], pool_weight.shape[1])
    mixed_groups = jnp.einsum(
        "tgc,gcd->tgd", grouped, pool_weight, preferred_element_type=jnp.float32
    )
    return (mixed_groups.reshape(row_total, local_width) * pool_scale).astype(jnp.bfloat16)


def route_ranks(group, groups):
    rows = group.shape[0]
    named = group[:, None] == jnp.arange(groups, dtype=jnp.int32)
    order = jnp.arange(rows, dtype=jnp.int32)
    before = (order[:, None] > order[None, :]).astype(jnp.bfloat16)
    earlier = jnp.dot(before, named.astype(jnp.bfloat16), preferred_element_type=jnp.float32)
    return jnp.sum(jnp.where(named, earlier, 0.0), axis=1).astype(jnp.int32)


def same_core(value, holders):
    peers = lax.axis_size("ep")
    rings = [list(range(c, peers, holders)) for c in range(holders)]
    return lax.all_to_all(value, "ep", 0, 0, axis_index_groups=rings, tiled=True)


def add_halves(own, lows, highs):
    half = lows[0].shape[0]

    def body(own_ref, *refs):
        out = refs[-1]
        for k, group in enumerate([refs[: len(lows)], refs[len(lows) : -1]]):
            rows = pl.ds(k * half, half)
            total = own_ref[rows].astype(jnp.float32)
            for ref in group:
                total = total + ref[...].astype(jnp.float32)
            out[rows] = total.astype(jnp.bfloat16)

    return pl.pallas_call(
        body, out_shape=jax.ShapeDtypeStruct(own.shape, jnp.bfloat16), name="add_halves"
    )(own, *lows, *highs)


def ring_sum(own, before_low, before_high, after_low, after_high, low, high):
    def joined(x, y):
        return (x.astype(jnp.float32) + y.astype(jnp.float32)).astype(jnp.bfloat16)

    low = turned(low, "tp", 1)
    high = turned(high, "tp", -1)
    after_high = turned(after_high, "tp", 1)
    before_low = turned(before_low, "tp", -1)
    after_low = turned(joined(after_low, low), "tp", 1)
    before_high = turned(joined(before_high, high), "tp", -1)
    return add_halves(own, [after_low, before_low], [after_high, before_high])


def expert_kernel(in_counts, out_counts, holders, local_experts, width, quarter):
    experts = holders * local_experts

    def body(*refs):
        ins, rest = refs[: len(in_counts)], refs[len(in_counts) :]
        weights, rest = rest[: 3 * holders], rest[3 * holders :]
        outs, rest = rest[: len(out_counts)], rest[len(out_counts) :]
        joined, both, downs, hidden, result, in_sem, up_sem, down_sem, out_sem = rest

        def row_copies(refs, counts, make):
            start = 0
            copies = []
            for k, count in enumerate(counts):
                copies.append(make(refs[k], start, count, k))
                start += count
            return copies

        entering = row_copies(
            ins,
            in_counts,
            lambda ref, start, count, k: pltpu.make_async_copy(
                ref, joined.at[pl.ds(start, count)], in_sem.at[k]
            ),
        )
        leaving = row_copies(
            outs,
            out_counts,
            lambda ref, start, count, k: pltpu.make_async_copy(
                result.at[pl.ds(start, count)], ref, out_sem.at[k]
            ),
        )
        lifts, lowers = [], []
        for e in range(experts):
            gate, up, down = weights[3 * (e // local_experts) : 3 * (e // local_experts) + 3]
            i = e % local_experts
            lifts.append(
                pltpu.make_async_copy(gate.at[i], both.at[e, :, pl.ds(0, quarter)], up_sem.at[0, e])
            )
            lifts.append(
                pltpu.make_async_copy(
                    up.at[i], both.at[e, :, pl.ds(quarter, quarter)], up_sem.at[1, e]
                )
            )
            lowers.append(pltpu.make_async_copy(down.at[i], downs.at[e], down_sem.at[e]))
        for copy in lifts[:2] + entering + lifts[2:] + lowers:
            copy.start()
        for copy in entering:
            copy.wait()

        def lift(e, carry):
            for k in range(2):
                part = both.at[e, :, pl.ds(k * quarter, quarter)]
                pltpu.make_async_copy(part, part, up_sem.at[k, e]).wait()

            def lift_rows(i, carry):
                rows = pl.ds(pl.multiple_of(i * lift_block, lift_block), lift_block)
                tail = joined[rows, width:].astype(jnp.float32)
                lane = lax.broadcasted_iota(jnp.int32, tail.shape, 1)
                mine = (lane == e) | (lane == e + GROUP_SIZE)
                weight = jnp.sum(jnp.where(mine, tail, 0.0), axis=1, keepdims=True)
                parts = jnp.dot(
                    joined[rows, :width], both[e], preferred_element_type=jnp.float32
                )
                gate_part = parts[:, :quarter]
                hidden[e, rows] = (
                    gate_part / (1.0 + jnp.exp(-gate_part)) * (parts[:, quarter:] * weight)
                ).astype(jnp.bfloat16)
                return carry

            return lax.fori_loop(0, joined.shape[0] // lift_block, lift_rows, carry)

        lax.fori_loop(0, experts, lift, 0)
        for copy in lowers:
            copy.wait()

        def lower(i, carry):
            rows = pl.ds(pl.multiple_of(i * lower_block, lower_block), lower_block)
            grouped = jnp.concatenate([hidden[e, rows] for e in range(experts)], axis=1)
            total = jnp.dot(
                grouped,
                downs[...].reshape(experts * quarter, width),
                preferred_element_type=jnp.float32,
            )
            result[rows] = total.astype(jnp.bfloat16)
            return carry

        lax.fori_loop(0, joined.shape[0] // lower_block, lower, 0)
        for copy in leaving:
            copy.start()
        for copy in leaving:
            copy.wait()

    return body


def expert_rows(rows, out_counts, sets):
    holders = len(sets)
    local_experts, width, quarter = sets[0][0].shape
    experts = holders * local_experts
    in_counts = [r.shape[0] for r in rows]
    total = sum(in_counts)
    full = rows[0].shape[1]
    anywhere = pl.BlockSpec(memory_space=pl.ANY)
    return pl.pallas_call(
        expert_kernel(in_counts, out_counts, holders, local_experts, width, quarter),
        in_specs=[anywhere] * (len(rows) + 3 * holders),
        out_specs=[anywhere] * len(out_counts),
        out_shape=[jax.ShapeDtypeStruct((count, width), jnp.bfloat16) for count in out_counts],
        scratch_shapes=[
            pltpu.VMEM((total, full), jnp.bfloat16),
            pltpu.VMEM((experts, width, 2 * quarter), jnp.bfloat16),
            pltpu.VMEM((experts, quarter, width), jnp.bfloat16),
            pltpu.VMEM((experts, total, quarter), jnp.bfloat16),
            pltpu.VMEM((total, width), jnp.bfloat16),
            pltpu.SemaphoreType.DMA((len(in_counts),)),
            pltpu.SemaphoreType.DMA((2, experts)),
            pltpu.SemaphoreType.DMA((experts,)),
            pltpu.SemaphoreType.DMA((len(out_counts),)),
        ],
        cost_estimate=pl.CostEstimate(
            flops=6 * total * width * quarter * experts,
            bytes_accessed=6 * width * quarter * experts + 2 * total * (full + width),
            transcendentals=total * quarter * experts,
        ),
        name="experts",
    )(*rows, *[w for one in sets for w in one])


def layer(
    mixer_tokens,
    mixer_gain,
    proj_in,
    pool_weight,
    pool_scale,
    proj_out,
    expert_tokens,
    expert_gain,
    expert_route,
    route_gate,
    expert_gate,
    expert_up,
    expert_down,
):
    ep_count = lax.axis_size("ep")
    tp_index = lax.axis_index("tp")
    ep_index = lax.axis_index("ep")
    own_count, model_width = mixer_tokens.shape
    local_width = proj_in.shape[1]
    group_width = pool_weight.shape[1]
    local_experts = expert_gate.shape[0]
    experts = local_experts * ep_count
    capacity = own_count * GROUP_SIZE // experts
    packet = capacity * GROUP_SIZE // 2
    groups = experts // GROUP_SIZE
    holders = GROUP_SIZE // local_experts
    place = ep_index % holders
    step = packet // chunks

    own_start = tp_index * own_count
    own_route = lax.dynamic_slice_in_dim(expert_route, own_start, own_count, 0)
    own_gates = lax.dynamic_slice_in_dim(route_gate, own_start, own_count, 0)
    group = own_route[:, 0] // GROUP_SIZE
    rank = route_ranks(group, groups)
    slot = rank // step * (groups * step) + group * step + rank % step
    pick = (
        slot[:, None] == jnp.arange(chunks * groups * step, dtype=jnp.int32)
    ).astype(jnp.bfloat16)

    member = (own_route - place * local_experts) % GROUP_SIZE
    lane = jnp.arange(extra, dtype=jnp.int32)
    by_lane = jnp.zeros((own_count, extra), jnp.float32)
    for k in range(2):
        hit = lane[None, :] % GROUP_SIZE == member[:, k : k + 1]
        by_lane = by_lane + jnp.where(hit, own_gates[:, k : k + 1], 0.0)
    high = lax.reduce_precision(by_lane, 8, 7)
    tail = jnp.where(
        lane < GROUP_SIZE, high, jnp.where(lane < 2 * GROUP_SIZE, by_lane - high, 0.0)
    ).astype(jnp.bfloat16)

    normed_expert = layer_norm(expert_tokens, expert_gain)
    extended = jnp.concatenate([normed_expert, tail], axis=1)
    outgoing = []
    for k in range(chunks):
        part = jnp.einsum(
            "ts,td->sd",
            pick[:, k * groups * step : (k + 1) * groups * step],
            extended,
            preferred_element_type=jnp.float32,
        ).astype(jnp.bfloat16)
        outgoing.append(part.reshape(groups, step, model_width + extra))

    outgoing[0], mixer_tokens, expert_gate, expert_up, expert_down = lax.optimization_barrier(
        (outgoing[0], mixer_tokens, expert_gate, expert_up, expert_down)
    )
    own_set = (expert_gate, expert_up, expert_down)
    sets = [own_set]
    for s in range(1, holders):
        pairs = [(i, i - i % holders + (i - s) % holders) for i in range(ep_count)]
        sets.append(tuple(lax.ppermute(w, "ep", pairs) for w in own_set))

    normed_mixer = layer_norm(mixer_tokens, mixer_gain)
    channel = tp_index * local_width + jnp.arange(local_width, dtype=jnp.int32)
    windows = jnp.left_shift(jnp.full_like(channel, 2), channel // group_width)
    gathered = spread(normed_mixer)

    partials = []
    back = []
    for k in range(chunks):
        arrived = same_core(outgoing[k], holders).reshape(-1, model_width + extra)
        rows = spread(arrived)
        count = arrived.shape[0]
        half = count // 2
        partials.append(expert_rows(rows, [count] + [half] * 6, sets))
        summed = ring_sum(*partials[k])
        back.append(same_core(summed.reshape(groups, step, model_width), holders))

    tp_count = lax.axis_size("tp")
    stacked = jnp.stack(gathered)
    blocks = jnp.dot(
        stacked.reshape(-1, model_width), proj_in, preferred_element_type=jnp.float32
    ).astype(jnp.bfloat16)
    blocks = blocks.reshape(tp_count, own_count, local_width)
    source_step = {s % tp_count: r for r, s in enumerate([0] + tp_steps())}
    by_distance = jnp.stack([blocks[source_step[d]] for d in range(tp_count)])
    order = (tp_index - jnp.arange(tp_count, dtype=jnp.int32)) % tp_count
    projected = by_distance[order].reshape(-1, local_width)
    pooled = pool_mix(
        projected, pool_weight, pool_scale, windows, ep_index * projected.shape[0]
    )
    product = jnp.dot(pooled, proj_out, preferred_element_type=jnp.float32).astype(
        jnp.bfloat16
    )
    product = product.reshape(tp_count, own_count, model_width)
    parts = [
        lax.dynamic_index_in_dim(product, (tp_index - s) % tp_count, 0, keepdims=False)
        for s in [0] + tp_steps()
    ]
    mixed_rows = collect(parts)

    total = None
    for k in range(chunks):
        part = jnp.dot(
            pick[:, k * groups * step : (k + 1) * groups * step],
            back[k].reshape(-1, model_width),
            preferred_element_type=jnp.float32,
        )
        total = part if total is None else total + part
    return (mixed_rows, total.astype(jnp.bfloat16))


def solution(mesh):
    return jax.shard_map(
        layer,
        mesh=mesh,
        in_specs=(
            P(("grp", "ep", "tp"), None),
            P(),
            P(None, "tp"),
            P("tp", None, None),
            P("tp"),
            P("tp", None),
            P(("grp", "ep", "tp"), None),
            P(),
            P(("grp", "ep"), None),
            P(("grp", "ep"), None),
            P("ep", None, "tp"),
            P("ep", None, "tp"),
            P("ep", "tp", None),
        ),
        out_specs=(P(("grp", "ep", "tp"), None), P(("grp", "ep", "tp"), None)),
        check_vma=False,
    )
```
